128 devices in a mesh: sp: 16 (over z, y), tp: 8 (over x, core).
Axes of the slice: x: 4, y: 4, z: 4, core: 2. Of those that a mesh axis runs over, the one named last changes fastest.
Arguments:
- residual_in: bfloat16 [16384, 2048], P(('sp', 'tp')), may hold values from -6 to 6
- queries: bfloat16 [16384, 2048], P('sp', 'tp'), may hold values from -6 to 6
- keys: bfloat16 [16384, 1024], P('sp', 'tp'), may hold values from -6 to 6
- values: bfloat16 [16384, 1024], P('sp', 'tp'), may hold values from -6 to 6
- query_gain: float32 [128], replicated, may hold values from 1 to 7
- key_norm_gain: float32 [128], replicated, may hold values from 1 to 7
- out_weight: bfloat16 [2048, 2048], replicated, may hold values from -0.125 to 0.125
- norm_gain: float32 [2048], replicated, may hold values from 0.1 to 1.9
- up_weight: bfloat16 [2048, 8192], P('sp', 'tp'), may hold values from -0.125 to 0.125
- down_weight: bfloat16 [8192, 2048], P('tp', 'sp'), may hold values from -0.0625 to 0.0625
Outputs:
- residual_out: bfloat16 [16384, 2048], P(('sp', 'tp'))
The draws below stay inside these ranges and needn't reach their ends.
All inputs are finite; a program needn't handle non-finite values.
Results may differ from the reference program's by a relative error of at most 0.017.
The reference program's roundings to bfloat16 on the way count: a program that leaves them out, or rounds other values in their place, can miss the bound.
Values may be sent and summed in bfloat16 or wider, within the bound.
No kernel may reach another device: no remote copies, remote signals or barrier semaphores. Data moves between devices by JAX's collectives and lax.ppermute only.
A program may use at most 128 MiB of HBM per device.

```python
import math
import jax
import jax.numpy as jnp
from jax import lax

D = 2048
FF = 8192
QUERY_HEADS = 16
KEY_VALUE_HEADS = 8
HEAD_WIDTH = 128
GRID_W = 64
SEQUENCE_TOKENS = 16384
N_TP = 8


def planted_pair(key):
    key_sample = jnp.clip(jax.random.normal(jax.random.fold_in(key, 11), (SEQUENCE_TOKENS, KEY_VALUE_HEADS * HEAD_WIDTH), jnp.float32), -6.0, 6.0)
    query_draw = jnp.clip(jax.random.normal(jax.random.fold_in(key, 12), (SEQUENCE_TOKENS, QUERY_HEADS * HEAD_WIDTH), jnp.float32), -6.0, 6.0)
    return (query_draw, key_sample)


def draw_queries(key, part):
    return planted_pair(key)[0].astype(jnp.bfloat16)


def draw_keys(key, part):
    return planted_pair(key)[1].astype(jnp.bfloat16)


def gain_draw(key):
    return jnp.clip(3.0 * (1.0 + 0.15 * jax.random.normal(key, (HEAD_WIDTH,), jnp.float32)), 1.0, 7.0)


def draw_query_gain(key, part):
    return gain_draw(jax.random.fold_in(key, 21))


def draw_key_norm_gain(key, part):
    return gain_draw(jax.random.fold_in(key, 22))


def block_scale(own_key, shape, pieces, least, high):
    level = 1.0
    for dim, parts in pieces:
        heights = jax.random.uniform(jax.random.fold_in(jax.random.fold_in(own_key, 6), dim), (parts,), jnp.float32, least / len(pieces), high / len(pieces))
        level = level * jnp.repeat(jnp.exp(heights), shape[dim] // parts).reshape((-1,) + (1,) * (len(shape) - 1 - dim))
    return level


def centred(rng, shape, scale, limit, split=(), held_as=jnp.bfloat16):
    values = jax.random.normal(rng, shape, jnp.float32) * scale
    if len(split) > 0:
        values = block_scale(rng, shape, split, -0.22, 0.18) * values
    return jnp.clip(values, min=-limit, max=limit).astype(held_as)


def setup_inputs(seed: int = 0) -> dict:
    arg_keys = jax.random.split(jax.random.key(seed), 11)
    residual_in = centred(arg_keys[0], (SEQUENCE_TOKENS, D), 1.0, 6.0, ((0, 128),))
    queries = draw_queries(jax.random.fold_in(arg_keys[10], 71), 0)
    keys = draw_keys(jax.random.fold_in(arg_keys[10], 71), 0)
    values = centred(arg_keys[3], (SEQUENCE_TOKENS, KEY_VALUE_HEADS * HEAD_WIDTH), 1.0, 6.0, ((0, 16), (1, 8)))
    query_gain = draw_query_gain(jax.random.fold_in(arg_keys[10], 71), 0)
    key_norm_gain = draw_key_norm_gain(jax.random.fold_in(arg_keys[10], 71), 0)
    out_weight = centred(arg_keys[6], (QUERY_HEADS * HEAD_WIDTH, D), (QUERY_HEADS * HEAD_WIDTH) ** -0.5, 0.125)
    norm_gain = jnp.clip(1.0 + 0.18 * jax.random.normal(arg_keys[7], (D,), jnp.float32), 0.1, 1.9)
    up_weight = centred(arg_keys[8], (D, FF), D ** -0.5, 0.125, ((0, 16), (1, 8)))
    down_weight = centred(arg_keys[9], (FF, D), FF ** -0.5, 0.0625, ((0, 8), (1, 16)))
    return {"residual_in": residual_in, "queries": queries, "keys": keys, "values": values, "query_gain": query_gain, "key_norm_gain": key_norm_gain, "out_weight": out_weight, "norm_gain": norm_gain, "up_weight": up_weight, "down_weight": down_weight}


epsilon = 1e-06

def rope_tables(count):
    places = jnp.arange(count)
    grid_row = (places // GRID_W).astype(jnp.float32)
    grid_col = (places % GRID_W).astype(jnp.float32)
    quarter = HEAD_WIDTH // 4
    inverse = 10000.0 ** (-jnp.arange(quarter, dtype=jnp.float32) / quarter)
    angle_row = grid_row[:, None] * inverse
    angle_col = grid_col[:, None] * inverse
    angles = jnp.concatenate([angle_row, angle_row, angle_col, angle_col], axis=-1)
    return (jnp.cos(angles), jnp.sin(angles))

def normalize_rotate(source, gain, heads, cosine_lookup, sine_lookup):
    count = source.shape[0]
    quarter = HEAD_WIDTH // 4
    vector = source.astype(jnp.float32).reshape(count, heads, HEAD_WIDTH)
    vector = vector * lax.rsqrt(lax.optimization_barrier(jnp.mean(vector * vector, axis=-1, keepdims=True)) + epsilon) * gain
    turned = jnp.concatenate([-vector[..., quarter:2 * quarter], vector[..., :quarter], -vector[..., 3 * quarter:], vector[..., 2 * quarter:3 * quarter]], axis=-1)
    rotated = vector * cosine_lookup[:, None, :] + turned * sine_lookup[:, None, :]
    return rotated.reshape(count, heads * HEAD_WIDTH).astype(jnp.bfloat16)

def reference(residual_in, queries, keys, values, query_gain, key_norm_gain, out_weight, norm_gain, up_weight, down_weight):
    cosine_lookup, sine_lookup = rope_tables(SEQUENCE_TOKENS)
    query_normalize = normalize_rotate(queries, query_gain, QUERY_HEADS, cosine_lookup, sine_lookup)
    key_normalize = normalize_rotate(keys, key_norm_gain, KEY_VALUE_HEADS, cosine_lookup, sine_lookup)
    queries_per_group = QUERY_HEADS // KEY_VALUE_HEADS
    key_lattice = key_normalize.astype(jnp.float32).reshape(SEQUENCE_TOKENS, KEY_VALUE_HEADS, HEAD_WIDTH)
    value_lattice = values.astype(jnp.float32).reshape(SEQUENCE_TOKENS, KEY_VALUE_HEADS, HEAD_WIDTH)
    rows_per_block = math.gcd(SEQUENCE_TOKENS, 256)
    query_tiles = query_normalize.reshape(SEQUENCE_TOKENS // rows_per_block, rows_per_block, KEY_VALUE_HEADS, queries_per_group, HEAD_WIDTH)

    def attend_block(query_block):
        scores = jnp.einsum('tkgd,rkd->tkgr', query_block.astype(jnp.float32), key_lattice) * HEAD_WIDTH ** (-0.5)
        highest = lax.optimization_barrier(jnp.max(scores, axis=-1, keepdims=True))
        weights = jnp.exp(scores - highest)
        denom = lax.optimization_barrier(jnp.sum(weights, axis=-1))
        rounded = lax.optimization_barrier(weights.astype(jnp.bfloat16)).astype(jnp.float32)
        summed = jnp.einsum('tkgr,rkd->tkgd', rounded, value_lattice)
        return (summed / denom[..., None]).astype(jnp.bfloat16)
    attn = lax.map(attend_block, query_tiles).reshape(SEQUENCE_TOKENS, QUERY_HEADS * HEAD_WIDTH)
    middle = residual_in.astype(jnp.float32) + jnp.dot(attn, out_weight, preferred_element_type=jnp.float32)
    normed = (middle * lax.rsqrt(lax.optimization_barrier(jnp.mean(middle * middle, axis=-1, keepdims=True)) + epsilon) * norm_gain).astype(jnp.bfloat16)
    hidden = jax.nn.relu(jnp.dot(normed, up_weight, preferred_element_type=jnp.float32))
    act = (hidden * hidden).astype(jnp.bfloat16)
    width = FF // N_TP
    down = jnp.zeros((SEQUENCE_TOKENS, D), jnp.float32)
    for block_index in range(N_TP):
        partial_sum = jnp.dot(act[:, block_index * width:(block_index + 1) * width], down_weight[block_index * width:(block_index + 1) * width], preferred_element_type=jnp.float32)
        down = down + lax.optimization_barrier(partial_sum.astype(jnp.bfloat16)).astype(jnp.float32)
    return (middle + down).astype(jnp.bfloat16)
```

```python
import functools
import numpy as np
import jax
import jax.numpy as jnp
from jax import lax
from jax.experimental import pallas as pl
from jax.experimental.pallas import tpu as pltpu
from jax.sharding import PartitionSpec as P

HEAD_WIDTH = 128
GRID_W = 64
epsilon = 1e-06

QB = 256
KB = 2048
SUB = 256
LOG2E = 1.4426950408889634
SCORE_SCALE = HEAD_WIDTH ** (-0.5) * LOG2E
ROWS = 144
LIMIT = 60 * 2**20


def rope_tables(tokens):
    quarter = HEAD_WIDTH // 4
    inverse = np.power(np.float32(10000.0), -np.arange(quarter, dtype=np.float32) / np.float32(quarter))

    def table(count, lane0):
        angle = (np.arange(count, dtype=np.float32)[:, None] * inverse.astype(np.float32)).astype(np.float64)
        cos = np.zeros((count, HEAD_WIDTH), np.float32)
        up = np.zeros((count, HEAD_WIDTH), np.float32)
        low = np.zeros((count, HEAD_WIDTH), np.float32)
        cos[:, lane0 : lane0 + quarter] = np.cos(angle)
        cos[:, lane0 + quarter : lane0 + 2 * quarter] = np.cos(angle)
        up[:, lane0 : lane0 + quarter] = -np.sin(angle)
        low[:, lane0 + quarter : lane0 + 2 * quarter] = np.sin(angle)
        return np.stack([cos, up, low])

    return table(tokens // GRID_W, 0), table(GRID_W, 2 * quarter)


def prep_kernel(sp_ref, q_ref, k_ref, v_ref, qg_ref, kg_ref, row_ref, col_ref, qt_ref, kv_ref, *, heads, step):
    del sp_ref
    grid_rows = step // GRID_W
    quarter = HEAD_WIDTH // 4

    def turn(x, gain, cos, up, low):
        y = x * lax.rsqrt(jnp.mean(x * x, axis=-1, keepdims=True) + epsilon) * gain
        return y * cos + pltpu.roll(y, HEAD_WIDTH - quarter, 1) * up + pltpu.roll(y, quarter, 1) * low

    for c in range(k_ref.shape[0] // step):
        at = slice(c * step, (c + 1) * step)
        tabs = []
        for n in range(3):
            both = row_ref[n, c * grid_rows : (c + 1) * grid_rows, :][:, None, :] + col_ref[n][None]
            tabs.append(both.reshape(step, HEAD_WIDTH))
        kn = turn(k_ref[at, :].astype(jnp.float32), kg_ref[...], *tabs)
        kv_ref[0, at, :] = kn.astype(jnp.bfloat16)
        for b in range(step // 128):
            rows = slice(c * step + b * 128, c * step + (b + 1) * 128)
            kv_ref[1, rows, :] = v_ref[rows, :].astype(jnp.float32).T.astype(jnp.bfloat16)
        for h in range(heads):
            x = q_ref[at, h * HEAD_WIDTH : (h + 1) * HEAD_WIDTH].astype(jnp.float32)
            qn = turn(x, qg_ref[...], *tabs)
            qt_ref[h * (k_ref.shape[0] // step) + c] = qn.T.astype(jnp.bfloat16)


def prep(queries, keys, values, query_gain, key_gain, sp_size):
    tokens = keys.shape[0]
    heads = queries.shape[1] // HEAD_WIDTH
    row_table, col_table = rope_tables(tokens * sp_size)
    rows = tokens // GRID_W
    where = jnp.reshape(lax.axis_index("sp").astype(jnp.int32), (1,))
    whole = lambda *shape: pl.BlockSpec(shape, lambda i, s: (0,) * len(shape))
    return pl.pallas_call(
        functools.partial(prep_kernel, heads=heads, step=QB),
        grid_spec=pltpu.PrefetchScalarGridSpec(
            num_scalar_prefetch=1,
            grid=(1,),
            in_specs=[
                whole(*queries.shape),
                whole(*keys.shape),
                whole(*values.shape),
                whole(1, HEAD_WIDTH),
                whole(1, HEAD_WIDTH),
                pl.BlockSpec((3, rows, HEAD_WIDTH), lambda i, s: (0, s[0], 0)),
                whole(3, GRID_W, HEAD_WIDTH),
            ],
            out_specs=[
                whole(heads * tokens // QB, HEAD_WIDTH, QB),
                whole(2, tokens, HEAD_WIDTH),
            ],
        ),
        out_shape=[
            jax.ShapeDtypeStruct((heads * tokens // QB, HEAD_WIDTH, QB), jnp.bfloat16),
            jax.ShapeDtypeStruct((2, tokens, HEAD_WIDTH), jnp.bfloat16),
        ],
        compiler_params=pltpu.CompilerParams(vmem_limit_bytes=LIMIT),
        name="prep",
    )(where, queries, keys, values, query_gain[None], key_gain[None], jnp.asarray(row_table), jnp.asarray(col_table))


def fold(x):
    for s in (4, 2, 1):
        x = jnp.maximum(x, pltpu.roll(x, s, 0))
    return x


def flash_kernel(*refs, n_q, n_kv, nt, nb):
    q_parts = refs[:n_q]
    kv_parts = refs[n_q : n_q + n_kv]
    o_ref, qs, ks, vs, q2, sa, sb, acc_ref, m_ref, sems = refs[n_q + n_kv :]
    copies = []
    at = 0
    for part in q_parts:
        copies.append((part, qs.at[pl.ds(at, part.shape[0])]))
        at += part.shape[0]
    at = 0
    for part in kv_parts:
        copies.append((part.at[0], ks.at[pl.ds(at, part.shape[1])]))
        copies.append((part.at[1], vs.at[pl.ds(at, part.shape[1])]))
        at += part.shape[1]
    copies = [pltpu.make_async_copy(a, b, sems.at[n]) for n, (a, b) in enumerate(copies)]
    for copy in copies:
        copy.start()
    for copy in copies:
        copy.wait()
    total = nt * nb

    def widen(t, carry):
        full = qs[t].astype(jnp.float32) * SCORE_SCALE
        high = full.astype(jnp.bfloat16)
        q2[t, :HEAD_WIDTH, :] = high
        q2[t, HEAD_WIDTH:, :] = (full - high.astype(jnp.float32)).astype(jnp.bfloat16)
        return carry

    lax.fori_loop(0, nt, widen, 0)

    def load_values(j, c):
        base = pl.multiple_of(j * KB + c * SUB, SUB)
        a = vs[pl.ds(base, 128), :]
        b = vs[pl.ds(base + 128, 128), :]
        v = jnp.concatenate([a, b], axis=1)
        return jnp.concatenate([v, jnp.ones((ROWS - HEAD_WIDTH, SUB), jnp.bfloat16)], axis=0)

    def scores(t, j, c):
        k = ks[pl.ds(pl.multiple_of(j * KB + c * SUB, SUB), SUB), :]
        return jnp.dot(jnp.concatenate([k, k], axis=1), q2[t], preferred_element_type=jnp.float32)

    def half(cur, nxt, i, block_max):
        t0, j0 = i // nb, i % nb
        i1 = jnp.minimum(i + 1, total - 1)
        t1, j1 = i1 // nb, i1 % nb
        first = j0 == 0
        m_old = jnp.where(first, jnp.full((8, QB), -1e30, jnp.float32), m_ref[t0])
        m_new = jnp.maximum(m_old, block_max)
        alpha = jnp.exp2(m_old - m_new)
        top = None
        delta = None
        for c in range(KB // SUB):
            sc = scores(t1, j1, c)
            nxt[c * SUB : (c + 1) * SUB, :] = sc
            mm = jnp.max(sc.reshape(SUB // 8, 8, QB), axis=0)
            top = mm if top is None else jnp.maximum(top, mm)
            p = jnp.exp2(cur[c * SUB : (c + 1) * SUB, :].reshape(SUB // 8, 8, QB) - m_new[None]).reshape(SUB, QB)
            d = jnp.dot(load_values(j0, c), p.astype(jnp.bfloat16), preferred_element_type=jnp.float32)
            delta = d if delta is None else delta + d
        acc = jnp.where(first, 0.0, acc_ref[t0])
        acc_ref[t0] = (acc.reshape(ROWS // 8, 8, QB) * alpha[None]).reshape(ROWS, QB) + delta
        m_ref[t0] = m_new
        return fold(top)

    top = None
    for c in range(KB // SUB):
        sc = scores(0, 0, c)
        sa[c * SUB : (c + 1) * SUB, :] = sc
        mm = jnp.max(sc.reshape(SUB // 8, 8, QB), axis=0)
        top = mm if top is None else jnp.maximum(top, mm)

    def body(h, block_max):
        block_max = half(sa, sb, 2 * h, block_max)
        return half(sb, sa, 2 * h + 1, block_max)

    lax.fori_loop(0, total // 2, body, fold(top))

    def finish(t, carry):
        a = acc_ref[t]
        mass = a[HEAD_WIDTH : HEAD_WIDTH + 1]
        o_ref[t, :HEAD_WIDTH, :] = (a[:HEAD_WIDTH] / mass).astype(jnp.bfloat16)
        lse = m_ref[t][:1] + jnp.log2(mass)
        high = lse.astype(jnp.bfloat16).astype(jnp.float32)
        mid = (lse - high).astype(jnp.bfloat16).astype(jnp.float32)
        low = lse - high - mid
        row = lax.broadcasted_iota(jnp.int32, (ROWS - HEAD_WIDTH, QB), 0)
        packed = jnp.where(row == 0, high, jnp.where(row == 1, mid, low))
        o_ref[t, HEAD_WIDTH:, :] = packed.astype(jnp.bfloat16)
        return carry

    lax.fori_loop(0, nt, finish, 0)


def flash(q_parts, kv_parts):
    nt = sum(q.shape[0] for q in q_parts)
    keys = sum(kv.shape[1] for kv in kv_parts)
    return pl.pallas_call(
        functools.partial(flash_kernel, n_q=len(q_parts), n_kv=len(kv_parts), nt=nt, nb=keys // KB),
        out_shape=jax.ShapeDtypeStruct((nt, ROWS, QB), jnp.bfloat16),
        in_specs=[pl.BlockSpec(memory_space=pl.ANY)] * (len(q_parts) + len(kv_parts)),
        out_specs=pl.BlockSpec(memory_space=pltpu.VMEM),
        scratch_shapes=[
            pltpu.VMEM((nt, HEAD_WIDTH, QB), jnp.bfloat16),
            pltpu.VMEM((keys, HEAD_WIDTH), jnp.bfloat16),
            pltpu.VMEM((keys, HEAD_WIDTH), jnp.bfloat16),
            pltpu.VMEM((nt, 2 * HEAD_WIDTH, QB), jnp.bfloat16),
            pltpu.VMEM((KB, QB), jnp.float32),
            pltpu.VMEM((KB, QB), jnp.float32),
            pltpu.VMEM((nt, ROWS, QB), jnp.float32),
            pltpu.VMEM((nt, 8, QB), jnp.float32),
            pltpu.SemaphoreType.DMA((len(q_parts) + 2 * len(kv_parts),)),
        ],
        cost_estimate=pl.CostEstimate(
            flops=4 * nt * QB * keys * HEAD_WIDTH * 2, bytes_accessed=2**22, transcendentals=nt * QB * keys
        ),
        compiler_params=pltpu.CompilerParams(vmem_limit_bytes=LIMIT),
        name="flash",
    )(*q_parts, *kv_parts)


def merge_kernel(*refs, n, tokens):
    parts, o_ref = refs[:n], refs[n]
    tiles = parts[0].shape[0]
    per_head = tokens // QB
    for t in range(tiles):
        lses = []
        for p in parts:
            tail = p[t, HEAD_WIDTH:, :].astype(jnp.float32)
            lses.append(tail[0:1] + tail[1:2] + tail[2:3])
        top = functools.reduce(jnp.maximum, lses)
        weights = [jnp.exp2(v - top) for v in lses]
        total = functools.reduce(jnp.add, weights)
        out = None
        for p, w in zip(parts, weights):
            term = p[t, :HEAD_WIDTH, :].astype(jnp.float32) * (w / total)
            out = term if out is None else out + term
        h, c = t // per_head, t % per_head
        o_ref[c * QB : (c + 1) * QB, h * HEAD_WIDTH : (h + 1) * HEAD_WIDTH] = out.T.astype(jnp.bfloat16)


def merge(parts, tokens, heads):
    return pl.pallas_call(
        functools.partial(merge_kernel, n=len(parts), tokens=tokens),
        out_shape=jax.ShapeDtypeStruct((tokens, heads * HEAD_WIDTH), jnp.bfloat16),
        in_specs=[pl.BlockSpec(memory_space=pltpu.VMEM)] * len(parts),
        out_specs=pl.BlockSpec(memory_space=pltpu.VMEM),
        compiler_params=pltpu.CompilerParams(vmem_limit_bytes=LIMIT),
        name="merge",
    )(*parts)


SIDE = 4


def sp_shift(dz, dy):
    return [
        (z * SIDE + y, ((z + dz) % SIDE) * SIDE + (y + dy) % SIDE) for z in range(SIDE) for y in range(SIDE)
    ]


def send(x, dz, dy):
    return lax.ppermute(x, "sp", sp_shift(dz, dy))


def local(
    residual_in,
    queries,
    keys,
    values,
    query_gain,
    key_norm_gain,
    out_weight,
    norm_gain,
    up_weight,
    down_weight,
    *,
    sp_size,
):
    tokens = keys.shape[0]
    heads = queries.shape[1] // HEAD_WIDTH
    q0, kv0 = prep(queries, keys, values, query_gain, key_norm_gain, sp_size)
    kv_p = send(kv0, 1, 0)
    q_p = send(q0, 0, 1)
    kv_m = send(kv0, -1, 0)
    q_m = send(q0, 0, -1)
    half_k, half_q = tokens // 2, q0.shape[0] // 2
    kv_2a = send(kv_p[:, :half_k], 1, 0)
    q_2a = send(q_p[:half_q], 0, 1)
    kv_2b = send(kv_m[:, half_k:], -1, 0)
    q_2b = send(q_m[half_q:], 0, -1)
    kv_all = [kv0, kv_p, kv_m, kv_2a, kv_2b]
    far = flash([q_2a, q_2b], kv_all)
    back_far = send(far, 0, 2)
    near_p = flash([q_p], kv_all)
    back_p = send(near_p, 0, -1)
    near_m = flash([q_m], kv_all)
    back_m = send(near_m, 0, 1)
    own = flash([q0], kv_all)
    attn = merge([own, back_p, back_m, back_far], tokens, heads)
    all_heads = lax.all_to_all(attn, "tp", split_axis=0, concat_axis=1, tiled=True)
    projected = jnp.dot(all_heads, out_weight, preferred_element_type=jnp.float32)
    middle = residual_in.astype(jnp.float32) + projected
    normed = (
        middle * lax.rsqrt(jnp.mean(middle * middle, axis=-1, keepdims=True) + epsilon) * norm_gain
    ).astype(jnp.bfloat16)
    whole_rows = lax.all_gather(normed, "tp", axis=0, tiled=True)
    hidden = jax.nn.relu(
        jnp.dot(
            whole_rows,
            lax.all_gather(up_weight, "sp", axis=0, tiled=True),
            preferred_element_type=jnp.float32,
        )
    )
    act = (hidden * hidden).astype(jnp.bfloat16)
    down_whole = lax.all_gather(down_weight, "sp", axis=1, tiled=True)
    down = lax.psum_scatter(
        jnp.dot(act, down_whole, preferred_element_type=jnp.float32).astype(jnp.bfloat16),
        "tp",
        scatter_dimension=0,
        tiled=True,
    ).astype(jnp.float32)
    return (middle + down).astype(jnp.bfloat16)


def solution(mesh):
    return jax.shard_map(
        functools.partial(local, sp_size=mesh.shape["sp"]),
        mesh=mesh,
        in_specs=(
            P(("sp", "tp"), None),
            P("sp", "tp"),
            P("sp", "tp"),
            P("sp", "tp"),
            P(),
            P(),
            P(),
            P(),
            P("sp", "tp"),
            P("tp", "sp"),
        ),
        out_specs=P(("sp", "tp"), None),
        check_vma=False,
    )
```

```python
import functools
import numpy as np
import jax
import jax.numpy as jnp
from jax import lax
from jax.experimental import pallas as pl
from jax.experimental.pallas import tpu as pltpu
from jax.sharding import PartitionSpec as P


HEAD_WIDTH = 128
GRID_W = 64
epsilon = 1e-06

QB = 256
SUB = 256
LOG2E = 1.4426950408889634
SCORE_SCALE = HEAD_WIDTH ** (-0.5) * LOG2E
ROWS = 144
LIMIT = 60 * 2**20


def rope_tables(tokens):
    quarter = HEAD_WIDTH // 4
    inverse = np.power(np.float32(10000.0), -np.arange(quarter, dtype=np.float32) / np.float32(quarter))

    def table(count, lane0):
        angle = (np.arange(count, dtype=np.float32)[:, None] * inverse.astype(np.float32)).astype(np.float64)
        cos = np.zeros((count, HEAD_WIDTH), np.float32)
        up = np.zeros((count, HEAD_WIDTH), np.float32)
        low = np.zeros((count, HEAD_WIDTH), np.float32)
        cos[:, lane0 : lane0 + quarter] = np.cos(angle)
        cos[:, lane0 + quarter : lane0 + 2 * quarter] = np.cos(angle)
        up[:, lane0 : lane0 + quarter] = -np.sin(angle)
        low[:, lane0 + quarter : lane0 + 2 * quarter] = np.sin(angle)
        return np.stack([cos, up, low])

    return table(tokens // GRID_W, 0), table(GRID_W, 2 * quarter)


def prep_kernel(
    sp_ref, q_ref, k_ref, v_ref, qg_ref, kg_ref, row_ref, col_ref, up_ref, down_ref, qt_ref, kv_ref, both_ref, *, heads, step
):
    del sp_ref
    each, width = up_ref.shape
    both_ref[:, :width] = up_ref[...]
    for n in range(down_ref.shape[0] // each):
        at = width + n * down_ref.shape[1]
        both_ref[:, at : at + down_ref.shape[1]] = down_ref[n * each : (n + 1) * each, :]
    grid_rows = step // GRID_W
    quarter = HEAD_WIDTH // 4

    def turn(x, gain, cos, up, low):
        y = x * lax.rsqrt(jnp.mean(x * x, axis=-1, keepdims=True) + epsilon) * gain
        return y * cos + pltpu.roll(y, HEAD_WIDTH - quarter, 1) * up + pltpu.roll(y, quarter, 1) * low

    for c in range(k_ref.shape[0] // step):
        at = slice(c * step, (c + 1) * step)
        tabs = []
        for n in range(3):
            both = row_ref[n, c * grid_rows : (c + 1) * grid_rows, :][:, None, :] + col_ref[n][None]
            tabs.append(both.reshape(step, HEAD_WIDTH))
        kn = turn(k_ref[at, :].astype(jnp.float32), kg_ref[...], *tabs)
        kv_ref[0, at, :] = kn.astype(jnp.bfloat16)
        for b in range(step // 128):
            rows = slice(c * step + b * 128, c * step + (b + 1) * 128)
            kv_ref[1, rows, :] = v_ref[rows, :].astype(jnp.float32).T.astype(jnp.bfloat16)
        for h in range(heads):
            x = q_ref[at, h * HEAD_WIDTH : (h + 1) * HEAD_WIDTH].astype(jnp.float32)
            qn = turn(x, qg_ref[...], *tabs)
            qt_ref[h * (k_ref.shape[0] // step) + c] = qn.T.astype(jnp.bfloat16)


def prep(queries, keys, values, query_gain, key_gain, up_weight, down_weight, sp_size):
    tokens = keys.shape[0]
    heads = queries.shape[1] // HEAD_WIDTH
    row_table, col_table = rope_tables(tokens * sp_size)
    rows = tokens // GRID_W
    where = jnp.reshape(lax.axis_index("sp").astype(jnp.int32), (1,))
    whole = lambda *shape: pl.BlockSpec(shape, lambda i, s: (0,) * len(shape))
    return pl.pallas_call(
        functools.partial(prep_kernel, heads=heads, step=QB),
        grid_spec=pltpu.PrefetchScalarGridSpec(
            num_scalar_prefetch=1,
            grid=(1,),
            in_specs=[
                whole(*queries.shape),
                whole(*keys.shape),
                whole(*values.shape),
                whole(1, HEAD_WIDTH),
                whole(1, HEAD_WIDTH),
                pl.BlockSpec((3, rows, HEAD_WIDTH), lambda i, s: (0, s[0], 0)),
                whole(3, GRID_W, HEAD_WIDTH),
                whole(*up_weight.shape),
                whole(*down_weight.shape),
            ],
            out_specs=[
                whole(heads * tokens // QB, HEAD_WIDTH, QB),
                whole(2, tokens, HEAD_WIDTH),
                whole(up_weight.shape[0], 2 * up_weight.shape[1]),
            ],
        ),
        out_shape=[
            jax.ShapeDtypeStruct((heads * tokens // QB, HEAD_WIDTH, QB), jnp.bfloat16),
            jax.ShapeDtypeStruct((2, tokens, HEAD_WIDTH), jnp.bfloat16),
            jax.ShapeDtypeStruct((up_weight.shape[0], 2 * up_weight.shape[1]), jnp.bfloat16),
        ],
        compiler_params=pltpu.CompilerParams(vmem_limit_bytes=LIMIT),
        name="prep",
    )(where, queries, keys, values, query_gain[None], key_gain[None], jnp.asarray(row_table), jnp.asarray(col_table), up_weight, down_weight)


def fold(x):
    for s in (4, 2, 1):
        x = jnp.maximum(x, pltpu.roll(x, s, 0))
    return x


def flash_kernel(*refs, n_q, n_kv, n_p, n_o, nt, nb, step):
    KB = step
    q_parts = refs[:n_q]
    kv_parts = refs[n_q : n_q + n_kv]
    priors = refs[n_q + n_kv : n_q + n_kv + n_p]
    o_refs = refs[n_q + n_kv + n_p : n_q + n_kv + n_p + n_o]
    qs, ks, vs, q2, sa, sb, acc_ref, m_ref, sems = refs[n_q + n_kv + n_p + n_o :]
    copies = []
    at = 0
    for part in q_parts:
        copies.append((part, qs.at[pl.ds(at, part.shape[0])]))
        at += part.shape[0]
    at = 0
    for part in kv_parts:
        copies.append((part.at[0], ks.at[pl.ds(at, part.shape[1])]))
        copies.append((part.at[1], vs.at[pl.ds(at, part.shape[1])]))
        at += part.shape[1]
    copies = [pltpu.make_async_copy(a, b, sems.at[n]) for n, (a, b) in enumerate(copies)]
    for copy in copies:
        copy.start()
    for copy in copies:
        copy.wait()
    total = nt * nb

    def widen(t, carry):
        full = qs[t].astype(jnp.float32) * SCORE_SCALE
        high = full.astype(jnp.bfloat16)
        q2[t, :HEAD_WIDTH, :] = high
        q2[t, HEAD_WIDTH:, :] = (full - high.astype(jnp.float32)).astype(jnp.bfloat16)
        return carry

    lax.fori_loop(0, nt, widen, 0)
    for n, prior in enumerate(priors):

        def resume(t, carry, n=n, prior=prior):
            at = n * prior.shape[0] + t
            tail = prior[t, HEAD_WIDTH:, :].astype(jnp.float32)
            acc_ref[at, :HEAD_WIDTH, :] = prior[t, :HEAD_WIDTH, :].astype(jnp.float32)
            acc_ref[at, HEAD_WIDTH:, :] = jnp.ones((ROWS - HEAD_WIDTH, QB), jnp.float32)
            m_ref[at] = jnp.broadcast_to(tail[0:1] + tail[1:2] + tail[2:3], (8, QB))
            return carry

        lax.fori_loop(0, prior.shape[0], resume, 0)

    def load_values(j, c):
        base = pl.multiple_of(j * KB + c * SUB, SUB)
        a = vs[pl.ds(base, 128), :]
        b = vs[pl.ds(base + 128, 128), :]
        v = jnp.concatenate([a, b], axis=1)
        return jnp.concatenate([v, jnp.ones((ROWS - HEAD_WIDTH, SUB), jnp.bfloat16)], axis=0)

    def scores(t, j, c):
        k = ks[pl.ds(pl.multiple_of(j * KB + c * SUB, SUB), SUB), :]
        return jnp.dot(jnp.concatenate([k, k], axis=1), q2[t], preferred_element_type=jnp.float32)

    def half(cur, nxt, i, block_max):
        t0, j0 = i // nb, i % nb
        i1 = jnp.minimum(i + 1, total - 1)
        t1, j1 = i1 // nb, i1 % nb
        if n_p:
            m_old = m_ref[t0]
        else:
            first = j0 == 0
            m_old = jnp.where(first, jnp.full((8, QB), -1e30, jnp.float32), m_ref[t0])
        m_new = jnp.maximum(m_old, block_max)
        alpha = jnp.exp2(m_old - m_new)
        top = None
        delta = None
        for c in range(KB // SUB):
            sc = scores(t1, j1, c)
            nxt[c * SUB : (c + 1) * SUB, :] = sc
            mm = jnp.max(sc.reshape(SUB // 8, 8, QB), axis=0)
            top = mm if top is None else jnp.maximum(top, mm)
            p = jnp.exp2(cur[c * SUB : (c + 1) * SUB, :].reshape(SUB // 8, 8, QB) - m_new[None]).reshape(SUB, QB)
            d = jnp.dot(load_values(j0, c), p.astype(jnp.bfloat16), preferred_element_type=jnp.float32)
            delta = d if delta is None else delta + d
        acc = acc_ref[t0] if n_p else jnp.where(first, 0.0, acc_ref[t0])
        acc_ref[t0] = (acc.reshape(ROWS // 8, 8, QB) * alpha[None]).reshape(ROWS, QB) + delta
        m_ref[t0] = m_new
        return fold(top)

    top = None
    for c in range(KB // SUB):
        sc = scores(0, 0, c)
        sa[c * SUB : (c + 1) * SUB, :] = sc
        mm = jnp.max(sc.reshape(SUB // 8, 8, QB), axis=0)
        top = mm if top is None else jnp.maximum(top, mm)

    def body(h, block_max):
        block_max = half(sa, sb, 2 * h, block_max)
        return half(sb, sa, 2 * h + 1, block_max)

    lax.fori_loop(0, total // 2, body, fold(top))

    each = nt // n_o
    for n, o_ref in enumerate(o_refs):

        def finish(t, carry, n=n, o_ref=o_ref):
            a = acc_ref[n * each + t]
            mass = a[HEAD_WIDTH : HEAD_WIDTH + 1]
            o_ref[t, :HEAD_WIDTH, :] = (a[:HEAD_WIDTH] / mass).astype(jnp.bfloat16)
            lse = m_ref[n * each + t][:1] + jnp.log2(mass)
            high = lse.astype(jnp.bfloat16).astype(jnp.float32)
            mid = (lse - high).astype(jnp.bfloat16).astype(jnp.float32)
            low = lse - high - mid
            row = lax.broadcasted_iota(jnp.int32, (ROWS - HEAD_WIDTH, QB), 0)
            packed = jnp.where(row == 0, high, jnp.where(row == 1, mid, low))
            o_ref[t, HEAD_WIDTH:, :] = packed.astype(jnp.bfloat16)
            return carry

        lax.fori_loop(0, each, finish, 0)


def flash(q_parts, kv_parts, n_o=1, priors=(), step=2048):
    nt = sum(q.shape[0] for q in q_parts)
    keys = sum(kv.shape[1] for kv in kv_parts)
    outs = pl.pallas_call(
        functools.partial(
            flash_kernel,
            n_q=len(q_parts),
            n_kv=len(kv_parts),
            n_p=len(priors),
            n_o=n_o,
            nt=nt,
            nb=keys // step,
            step=step,
        ),
        out_shape=[jax.ShapeDtypeStruct((nt // n_o, ROWS, QB), jnp.bfloat16)] * n_o,
        in_specs=[pl.BlockSpec(memory_space=pltpu.HBM)] * (len(q_parts) + len(kv_parts))
        + [pl.BlockSpec(memory_space=pltpu.VMEM)] * len(priors),
        out_specs=[pl.BlockSpec(memory_space=pltpu.VMEM)] * n_o,
        scratch_shapes=[
            pltpu.VMEM((nt, HEAD_WIDTH, QB), jnp.bfloat16),
            pltpu.VMEM((keys, HEAD_WIDTH), jnp.bfloat16),
            pltpu.VMEM((keys, HEAD_WIDTH), jnp.bfloat16),
            pltpu.VMEM((nt, 2 * HEAD_WIDTH, QB), jnp.bfloat16),
            pltpu.VMEM((step, QB), jnp.float32),
            pltpu.VMEM((step, QB), jnp.float32),
            pltpu.VMEM((nt, ROWS, QB), jnp.float32),
            pltpu.VMEM((nt, 8, QB), jnp.float32),
            pltpu.SemaphoreType.DMA((len(q_parts) + 2 * len(kv_parts),)),
        ],
        cost_estimate=pl.CostEstimate(
            flops=4 * nt * QB * keys * HEAD_WIDTH * 2, bytes_accessed=2**22, transcendentals=nt * QB * keys
        ),
        compiler_params=pltpu.CompilerParams(vmem_limit_bytes=LIMIT),
        name="flash",
    )(*q_parts, *kv_parts, *priors)
    return outs if n_o > 1 else outs[0]


def merge_kernel(*refs, n, tokens):
    parts, o_ref = refs[:n], refs[n]
    tiles = parts[0].shape[0]
    per_head = tokens // QB
    for t in range(tiles):
        lses = []
        for p in parts:
            tail = p[t, HEAD_WIDTH:, :].astype(jnp.float32)
            lses.append(tail[0:1] + tail[1:2] + tail[2:3])
        top = functools.reduce(jnp.maximum, lses)
        weights = [jnp.exp2(v - top) for v in lses]
        total = functools.reduce(jnp.add, weights)
        out = None
        for p, w in zip(parts, weights):
            term = p[t, :HEAD_WIDTH, :].astype(jnp.float32) * (w / total)
            out = term if out is None else out + term
        h, c = t // per_head, t % per_head
        o_ref[c * QB : (c + 1) * QB, h * HEAD_WIDTH : (h + 1) * HEAD_WIDTH] = out.T.astype(jnp.bfloat16)


def merge(parts, tokens, heads):
    return pl.pallas_call(
        functools.partial(merge_kernel, n=len(parts), tokens=tokens),
        out_shape=jax.ShapeDtypeStruct((tokens, heads * HEAD_WIDTH), jnp.bfloat16),
        in_specs=[pl.BlockSpec(memory_space=pltpu.VMEM)] * len(parts),
        out_specs=pl.BlockSpec(memory_space=pltpu.VMEM),
        compiler_params=pltpu.CompilerParams(vmem_limit_bytes=LIMIT),
        name="merge",
    )(*parts)


SIDE = 4


def sp_shift(dz, dy):
    return [
        (z * SIDE + y, ((z + dz) % SIDE) * SIDE + (y + dy) % SIDE) for z in range(SIDE) for y in range(SIDE)
    ]


def send(x, dz, dy):
    return lax.ppermute(x, "sp", sp_shift(dz, dy))


def front_kernel(at_ref, attn_ref, *refs, blocks, members):
    res_refs = refs[:members]
    wo_ref, gain_ref, own_ref, other_ref, act_ref, mid_out_ref, lhs, mid = refs[members:]
    i = pl.program_id(0)
    parts, _, each, width = attn_ref.shape
    _, model = lhs.shape
    block = model // blocks

    @pl.when(i == 0)
    def _():
        for m in range(members):
            source = (at_ref[1] + m) % members
            for p in range(parts):
                lhs[m * each : (m + 1) * each, p * width : (p + 1) * width] = attn_ref[p, source]

    @pl.when(i < blocks)
    def _():
        product = jnp.dot(lhs[...], wo_ref[...], preferred_element_type=jnp.float32)
        for m, res in enumerate(res_refs):
            at = slice(m * each, (m + 1) * each)
            mid[i, at, :] = res[...].astype(jnp.float32) + product[at]

    @pl.when(i == blocks)
    def _():
        for r in range(members):
            at = slice(r * each, (r + 1) * each)
            squares = None
            for n in range(blocks):
                for c in range(block // 128):
                    m = mid[n, at, c * 128 : (c + 1) * 128]
                    squares = m * m if squares is None else squares + m * m
            scale = lax.rsqrt(jnp.sum(squares, axis=-1, keepdims=True) * (1.0 / model) + epsilon)
            for n in range(blocks):
                gain = gain_ref[:, n * block : (n + 1) * block]
                lhs[at, n * block : (n + 1) * block] = (mid[n, at, :] * scale * gain).astype(jnp.bfloat16)
        for n in range(blocks):
            mid_out_ref[:, n * block : (n + 1) * block] = mid[n, :each, :]

    def hidden(g_ref):
        h = jnp.dot(lhs[...], g_ref[...].reshape(model, block), preferred_element_type=jnp.float32)
        h = jnp.maximum(h, 0.0)
        act_ref[...] = (h * h).astype(jnp.bfloat16).reshape(members, each, block)

    @pl.when((i >= blocks) & (i < blocks + blocks // 2))
    def _():
        hidden(own_ref)

    @pl.when(i >= blocks + blocks // 2)
    def _():
        hidden(other_ref)


def front(where, attn, residuals, out_weight, norm_gain, own, other, blocks=4):
    parts, members, _, each, width = attn.shape
    model = out_weight.shape[1]
    rows = members * each
    block = model // blocks
    half = blocks // 2
    weight = lambda first: pl.BlockSpec(
        (own.shape[0], each, block), lambda i, a: (0, 0, jnp.clip(i - first, 0, half - 1))
    )
    return pl.pallas_call(
        functools.partial(front_kernel, blocks=blocks, members=members),
        grid_spec=pltpu.PrefetchScalarGridSpec(
            num_scalar_prefetch=1,
            grid=(2 * blocks,),
            in_specs=[
                pl.BlockSpec((parts, members, None, each, width), lambda i, a: (0, 0, a[0], 0, 0)),
            ]
            + [pl.BlockSpec((each, block), lambda i, a: (0, jnp.minimum(i, blocks - 1)))] * members
            + [
                pl.BlockSpec((model, block), lambda i, a: (0, jnp.minimum(i, blocks - 1))),
                pl.BlockSpec((1, model), lambda i, a: (0, 0)),
                weight(blocks),
                weight(blocks + half),
            ],
            out_specs=[
                pl.BlockSpec((members, each, block), lambda i, a: (0, 0, jnp.maximum(i - blocks, 0))),
                pl.BlockSpec((each, model), lambda i, a: (0, 0)),
            ],
            scratch_shapes=[
                pltpu.VMEM((rows, model), jnp.bfloat16),
                pltpu.VMEM((blocks, rows, block), jnp.float32),
            ],
        ),
        out_shape=[
            jax.ShapeDtypeStruct((members, each, blocks * block), jnp.bfloat16),
            jax.ShapeDtypeStruct((each, model), jnp.float32),
        ],
        compiler_params=pltpu.CompilerParams(vmem_limit_bytes=LIMIT),
        name="front",
    )(where, attn, *residuals, out_weight, norm_gain[None], own, other)


def down_kernel(*refs, n_act, n_out):
    act_refs = refs[:n_act]
    own_ref, other_ref = refs[n_act : n_act + 2]
    o_refs = refs[n_act + 2 : n_act + 2 + n_out]
    lhs, w_ref = refs[n_act + 2 + n_out :]
    each = act_refs[0].shape[0]
    half = lhs.shape[1] // 2
    shards = own_ref.shape[0]

    @pl.when(pl.program_id(0) == 0)
    def _():
        for n, act_ref in enumerate(act_refs):
            lhs[n * each : (n + 1) * each, :] = act_ref[...]

    for n, g_ref in enumerate((own_ref, other_ref)):
        for b in range(half // 128):
            for j in range(shards):
                at = slice(n * half + b * 128, n * half + (b + 1) * 128)
                w_ref[at, j * 128 : (j + 1) * 128] = g_ref[j, :, b * 128 : (b + 1) * 128]
    product = jnp.dot(lhs[...], w_ref[...], preferred_element_type=jnp.float32).astype(jnp.bfloat16)
    rows = lhs.shape[0] // n_out
    for n, o_ref in enumerate(o_refs):
        o_ref[...] = product[n * rows : (n + 1) * rows]


def down(act, picks, own, other, n_out, group=4):
    _, each, width = act.shape
    shards, _, both = own.shape
    rows = len(picks) * each // n_out
    spec = pl.BlockSpec((group, each, both // 2), lambda i: (i, 0, 1))
    return pl.pallas_call(
        functools.partial(down_kernel, n_act=len(picks), n_out=n_out),
        grid=(shards // group,),
        in_specs=[pl.BlockSpec((None, each, width), lambda i, p=p: (p, 0, 0)) for p in picks] + [spec, spec],
        out_specs=[pl.BlockSpec((rows, group * each), lambda i: (0, i))] * n_out,
        out_shape=[jax.ShapeDtypeStruct((rows, shards * each), jnp.bfloat16)] * n_out,
        scratch_shapes=[
            pltpu.VMEM((len(picks) * each, width), jnp.bfloat16),
            pltpu.VMEM((width, group * each), jnp.bfloat16),
        ],
        compiler_params=pltpu.CompilerParams(vmem_limit_bytes=LIMIT),
        name="down",
    )(*[act] * len(picks), own, other)


def local(
    residual_in,
    queries,
    keys,
    values,
    query_gain,
    key_norm_gain,
    out_weight,
    norm_gain,
    up_weight,
    down_weight,
    *,
    sp_size,
    tp_size,
):
    tokens = keys.shape[0]
    heads = queries.shape[1] // HEAD_WIDTH
    mine = residual_in.shape[0]
    chips = tp_size // 2

    def send_x(x, dx):
        pairs = [(t, (t + 2 * dx) % tp_size) for t in range(tp_size)]
        return lax.ppermute(x, "tp", pairs)

    q0, kv0, both = prep(
        queries, keys, values, query_gain, key_norm_gain, up_weight, down_weight, sp_size
    )
    kv_p = send(kv0, 1, 0)
    kv_m = send(kv0, -1, 0)
    q_p = send(q0, 0, 1)
    q_m = send(q0, 0, -1)
    weights = lax.all_gather(both, "sp", axis=0)
    residuals = [residual_in] + [send_x(residual_in, -d) for d in (1, 2, 3)]
    own = flash([q0], [kv0], step=1024)
    half_k, half_q = tokens // 2, q0.shape[0] // 2
    kv_2a = send(kv_p[:, :half_k], 1, 0)
    kv_2b = send(kv_m[:, half_k:], -1, 0)
    q_2a = send(q_p[:half_q], 0, 1)
    q_2b = send(q_m[half_q:], 0, -1)
    near_p, near_m = flash([q_p, q_m], [kv0, kv_p, kv_m], 2, step=3072)
    q_2a, near_p = lax.optimization_barrier((q_2a, near_p))
    far = flash([q_2a, q_2b], [kv0, kv_p, kv_m, kv_2a, kv_2b], step=4096)
    back_far = send(far, 0, 2)
    near_p, far = lax.optimization_barrier((near_p, far))
    near_p, near_m = flash([q_p, q_m], [kv_2a, kv_2b], 2, (near_p, near_m), step=1024)
    back_p = send(near_p, 0, -1)
    back_m = send(near_m, 0, 1)
    own, near_p = lax.optimization_barrier((own, near_p))
    own = flash([q0], [kv_p, kv_m, kv_2a, kv_2b], 1, (own,), step=3072)
    weights, own = lax.optimization_barrier((weights, own))
    other_weights = lax.ppermute(weights, "tp", [(t, t ^ 1) for t in range(tp_size)])
    attn = merge([own, back_p, back_m, back_far], tokens, heads)
    all_heads = lax.all_gather(attn, "tp", axis=0)
    all_heads = all_heads.reshape(tp_size, chips, 2, mine, heads * HEAD_WIDTH)
    index = lax.axis_index("tp").astype(jnp.int32)
    where = jnp.stack([index % 2, index // 2])
    act, middle = front(where, all_heads, residuals, out_weight, norm_gain, weights, other_weights)
    far_sum = down(act, [2], weights, other_weights, 1)[0]
    from_far = send_x(far_sum, 2)
    far_sum, act = lax.optimization_barrier((far_sum, act))
    mine_sum, up_sum, low_sum = down(act, [0, 1, 3], weights, other_weights, 3)
    wide = lambda x: x.astype(jnp.float32)
    from_low = send_x(up_sum, 1)
    from_up = send_x(low_sum, -1)
    return (middle + wide(mine_sum) + wide(from_low) + wide(from_up) + wide(from_far)).astype(jnp.bfloat16)


def solution(mesh):
    return jax.shard_map(
        functools.partial(local, sp_size=mesh.shape["sp"], tp_size=mesh.shape["tp"]),
        mesh=mesh,
        in_specs=(
            P(("sp", "tp"), None),
            P("sp", "tp"),
            P("sp", "tp"),
            P("sp", "tp"),
            P(),
            P(),
            P(),
            P(),
            P("sp", "tp"),
            P("tp", "sp"),
        ),
        out_specs=P(("sp", "tp"), None),
        check_vma=False,
    )
```

```python
import functools
import numpy as np
import jax
import jax.numpy as jnp
from jax import lax
from jax.experimental import pallas as pl
from jax.experimental.pallas import tpu as pltpu
from jax.sharding import PartitionSpec as P


HEAD_WIDTH = 128
GRID_W = 64
epsilon = 1e-06

QB = 256
SUB = 512
LOG2E = 1.4426950408889634
SCORE_SCALE = HEAD_WIDTH ** (-0.5) * LOG2E
ROWS = 144
LIMIT = 60 * 2**20


def rope_tables(tokens):
    quarter = HEAD_WIDTH // 4
    inverse = np.power(np.float32(10000.0), -np.arange(quarter, dtype=np.float32) / np.float32(quarter))

    def table(count, lane0):
        angle = (np.arange(count, dtype=np.float32)[:, None] * inverse.astype(np.float32)).astype(np.float64)
        cos = np.zeros((count, HEAD_WIDTH), np.float32)
        up = np.zeros((count, HEAD_WIDTH), np.float32)
        low = np.zeros((count, HEAD_WIDTH), np.float32)
        cos[:, lane0 : lane0 + quarter] = np.cos(angle)
        cos[:, lane0 + quarter : lane0 + 2 * quarter] = np.cos(angle)
        up[:, lane0 : lane0 + quarter] = -np.sin(angle)
        low[:, lane0 + quarter : lane0 + 2 * quarter] = np.sin(angle)
        return np.stack([cos, up, low])

    return table(tokens // GRID_W, 0), table(GRID_W, 2 * quarter)


def prep_kernel(
    sp_ref, q_ref, k_ref, v_ref, qg_ref, kg_ref, row_ref, col_ref, up_ref, down_ref, qt_ref, kv_ref, both_ref, *, heads, step
):
    del sp_ref
    each, width = up_ref.shape
    both_ref[:, :width] = up_ref[...]
    for n in range(down_ref.shape[0] // each):
        at = width + n * down_ref.shape[1]
        both_ref[:, at : at + down_ref.shape[1]] = down_ref[n * each : (n + 1) * each, :]
    grid_rows = step // GRID_W
    quarter = HEAD_WIDTH // 4

    def turn(x, gain, cos, up, low):
        y = x * lax.rsqrt(jnp.mean(x * x, axis=-1, keepdims=True) + epsilon) * gain
        return y * cos + pltpu.roll(y, HEAD_WIDTH - quarter, 1) * up + pltpu.roll(y, quarter, 1) * low

    for c in range(k_ref.shape[0] // step):
        at = slice(c * step, (c + 1) * step)
        tabs = []
        for n in range(3):
            both = row_ref[n, c * grid_rows : (c + 1) * grid_rows, :][:, None, :] + col_ref[n][None]
            tabs.append(both.reshape(step, HEAD_WIDTH))
        kn = turn(k_ref[at, :].astype(jnp.float32), kg_ref[...], *tabs)
        kv_ref[0, at, :] = kn.astype(jnp.bfloat16)
        for b in range(step // 128):
            rows = slice(c * step + b * 128, c * step + (b + 1) * 128)
            kv_ref[1, rows, :] = v_ref[rows, :].astype(jnp.float32).T.astype(jnp.bfloat16)
        for h in range(heads):
            x = q_ref[at, h * HEAD_WIDTH : (h + 1) * HEAD_WIDTH].astype(jnp.float32)
            qn = turn(x, qg_ref[...], *tabs)
            qt_ref[h * (k_ref.shape[0] // step) + c] = qn.T.astype(jnp.bfloat16)


def prep(queries, keys, values, query_gain, key_gain, up_weight, down_weight, sp_size):
    tokens = keys.shape[0]
    heads = queries.shape[1] // HEAD_WIDTH
    row_table, col_table = rope_tables(tokens * sp_size)
    rows = tokens // GRID_W
    where = jnp.reshape(lax.axis_index("sp").astype(jnp.int32), (1,))
    whole = lambda *shape: pl.BlockSpec(shape, lambda i, s: (0,) * len(shape))
    return pl.pallas_call(
        functools.partial(prep_kernel, heads=heads, step=QB),
        grid_spec=pltpu.PrefetchScalarGridSpec(
            num_scalar_prefetch=1,
            grid=(1,),
            in_specs=[
                whole(*queries.shape),
                whole(*keys.shape),
                whole(*values.shape),
                whole(1, HEAD_WIDTH),
                whole(1, HEAD_WIDTH),
                pl.BlockSpec((3, rows, HEAD_WIDTH), lambda i, s: (0, s[0], 0)),
                whole(3, GRID_W, HEAD_WIDTH),
                whole(*up_weight.shape),
                whole(*down_weight.shape),
            ],
            out_specs=[
                whole(heads * tokens // QB, HEAD_WIDTH, QB),
                whole(2, tokens, HEAD_WIDTH),
                whole(up_weight.shape[0], 2 * up_weight.shape[1]),
            ],
        ),
        out_shape=[
            jax.ShapeDtypeStruct((heads * tokens // QB, HEAD_WIDTH, QB), jnp.bfloat16),
            jax.ShapeDtypeStruct((2, tokens, HEAD_WIDTH), jnp.bfloat16),
            jax.ShapeDtypeStruct((up_weight.shape[0], 2 * up_weight.shape[1]), jnp.bfloat16),
        ],
        compiler_params=pltpu.CompilerParams(vmem_limit_bytes=LIMIT),
        name="prep",
    )(where, queries, keys, values, query_gain[None], key_gain[None], jnp.asarray(row_table), jnp.asarray(col_table), up_weight, down_weight)


def fold(x):
    for s in (4, 2, 1):
        x = jnp.maximum(x, pltpu.roll(x, s, 0))
    return x


def flash_kernel(*refs, n_q, n_kv, n_p, n_o, nt, nb, step):
    KB = step
    q_parts = refs[:n_q]
    kv_parts = refs[n_q : n_q + n_kv]
    priors = refs[n_q + n_kv : n_q + n_kv + n_p]
    o_refs = refs[n_q + n_kv + n_p : n_q + n_kv + n_p + n_o]
    qs, ks, vs, q2, sa, sb, acc_ref, m_ref, sems = refs[n_q + n_kv + n_p + n_o :]
    copies = []
    at = 0
    for part in q_parts:
        copies.append((part, qs.at[pl.ds(at, part.shape[0])]))
        at += part.shape[0]
    at = 0
    for part in kv_parts:
        copies.append((part.at[0], ks.at[pl.ds(at, part.shape[1])]))
        copies.append((part.at[1], vs.at[pl.ds(at, part.shape[1])]))
        at += part.shape[1]
    copies = [pltpu.make_async_copy(a, b, sems.at[n]) for n, (a, b) in enumerate(copies)]
    for copy in copies:
        copy.start()
    for copy in copies:
        copy.wait()
    total = nt * nb

    def widen(t, carry):
        full = qs[t].astype(jnp.float32) * SCORE_SCALE
        high = full.astype(jnp.bfloat16)
        q2[t, :HEAD_WIDTH, :] = high
        q2[t, HEAD_WIDTH:, :] = (full - high.astype(jnp.float32)).astype(jnp.bfloat16)
        return carry

    lax.fori_loop(0, nt, widen, 0)
    for n, prior in enumerate(priors):

        def resume(t, carry, n=n, prior=prior):
            at = n * prior.shape[0] + t
            tail = prior[t, HEAD_WIDTH:, :].astype(jnp.float32)
            acc_ref[at, :HEAD_WIDTH, :] = prior[t, :HEAD_WIDTH, :].astype(jnp.float32)
            acc_ref[at, HEAD_WIDTH:, :] = jnp.ones((ROWS - HEAD_WIDTH, QB), jnp.float32)
            m_ref[at] = jnp.broadcast_to(tail[0:1] + tail[1:2] + tail[2:3], (8, QB))
            return carry

        lax.fori_loop(0, prior.shape[0], resume, 0)

    def load_values(j, c):
        base = pl.multiple_of(j * KB + c * SUB, SUB)
        v = jnp.concatenate([vs[pl.ds(base + n, 128), :] for n in range(0, SUB, 128)], axis=1)
        return jnp.concatenate([v, jnp.ones((ROWS - HEAD_WIDTH, SUB), jnp.bfloat16)], axis=0)

    def scores(t, j, c):
        k = ks[pl.ds(pl.multiple_of(j * KB + c * SUB, SUB), SUB), :]
        return jnp.dot(jnp.concatenate([k, k], axis=1), q2[t], preferred_element_type=jnp.float32)

    def half(cur, nxt, i, block_max):
        t0, j0 = i // nb, i % nb
        i1 = jnp.minimum(i + 1, total - 1)
        t1, j1 = i1 // nb, i1 % nb
        if n_p:
            m_old = m_ref[t0]
        else:
            first = j0 == 0
            m_old = jnp.where(first, jnp.full((8, QB), -1e30, jnp.float32), m_ref[t0])
        m_new = jnp.maximum(m_old, block_max)
        alpha = jnp.exp2(m_old - m_new)
        top = None
        delta = None
        for c in range(KB // SUB):
            sc = scores(t1, j1, c)
            nxt[c * SUB : (c + 1) * SUB, :] = sc
            mm = jnp.max(sc.reshape(SUB // 8, 8, QB), axis=0)
            top = mm if top is None else jnp.maximum(top, mm)
            p = jnp.exp2(cur[c * SUB : (c + 1) * SUB, :].reshape(SUB // 8, 8, QB) - m_new[None]).reshape(SUB, QB)
            d = jnp.dot(load_values(j0, c), p.astype(jnp.bfloat16), preferred_element_type=jnp.float32)
            delta = d if delta is None else delta + d
        acc = acc_ref[t0] if n_p else jnp.where(first, 0.0, acc_ref[t0])
        acc_ref[t0] = (acc.reshape(ROWS // 8, 8, QB) * alpha[None]).reshape(ROWS, QB) + delta
        m_ref[t0] = m_new
        return fold(top)

    top = None
    for c in range(KB // SUB):
        sc = scores(0, 0, c)
        sa[c * SUB : (c + 1) * SUB, :] = sc
        mm = jnp.max(sc.reshape(SUB // 8, 8, QB), axis=0)
        top = mm if top is None else jnp.maximum(top, mm)

    def body(h, block_max):
        block_max = half(sa, sb, 2 * h, block_max)
        return half(sb, sa, 2 * h + 1, block_max)

    lax.fori_loop(0, total // 2, body, fold(top))

    each = nt // n_o
    for n, o_ref in enumerate(o_refs):

        def finish(t, carry, n=n, o_ref=o_ref):
            a = acc_ref[n * each + t]
            mass = a[HEAD_WIDTH : HEAD_WIDTH + 1]
            o_ref[t, :HEAD_WIDTH, :] = (a[:HEAD_WIDTH] / mass).astype(jnp.bfloat16)
            lse = m_ref[n * each + t][:1] + jnp.log2(mass)
            high = lse.astype(jnp.bfloat16).astype(jnp.float32)
            mid = (lse - high).astype(jnp.bfloat16).astype(jnp.float32)
            low = lse - high - mid
            row = lax.broadcasted_iota(jnp.int32, (ROWS - HEAD_WIDTH, QB), 0)
            packed = jnp.where(row == 0, high, jnp.where(row == 1, mid, low))
            o_ref[t, HEAD_WIDTH:, :] = packed.astype(jnp.bfloat16)
            return carry

        lax.fori_loop(0, each, finish, 0)


def flash(q_parts, kv_parts, n_o=1, priors=(), step=2048):
    nt = sum(q.shape[0] for q in q_parts)
    keys = sum(kv.shape[1] for kv in kv_parts)
    outs = pl.pallas_call(
        functools.partial(
            flash_kernel,
            n_q=len(q_parts),
            n_kv=len(kv_parts),
            n_p=len(priors),
            n_o=n_o,
            nt=nt,
            nb=keys // step,
            step=step,
        ),
        out_shape=[jax.ShapeDtypeStruct((nt // n_o, ROWS, QB), jnp.bfloat16)] * n_o,
        in_specs=[pl.BlockSpec(memory_space=pltpu.HBM)] * (len(q_parts) + len(kv_parts))
        + [pl.BlockSpec(memory_space=pltpu.VMEM)] * len(priors),
        out_specs=[pl.BlockSpec(memory_space=pltpu.VMEM)] * n_o,
        scratch_shapes=[
            pltpu.VMEM((nt, HEAD_WIDTH, QB), jnp.bfloat16),
            pltpu.VMEM((keys, HEAD_WIDTH), jnp.bfloat16),
            pltpu.VMEM((keys, HEAD_WIDTH), jnp.bfloat16),
            pltpu.VMEM((nt, 2 * HEAD_WIDTH, QB), jnp.bfloat16),
            pltpu.VMEM((step, QB), jnp.float32),
            pltpu.VMEM((step, QB), jnp.float32),
            pltpu.VMEM((nt, ROWS, QB), jnp.float32),
            pltpu.VMEM((nt, 8, QB), jnp.float32),
            pltpu.SemaphoreType.DMA((len(q_parts) + 2 * len(kv_parts),)),
        ],
        cost_estimate=pl.CostEstimate(
            flops=4 * nt * QB * keys * HEAD_WIDTH * 2, bytes_accessed=2**22, transcendentals=nt * QB * keys
        ),
        compiler_params=pltpu.CompilerParams(vmem_limit_bytes=LIMIT),
        name="flash",
    )(*q_parts, *kv_parts, *priors)
    return outs if n_o > 1 else outs[0]


def merge_kernel(at_ref, *refs, n):
    parts, same_ref, other_ref = refs[:n], refs[n], refs[n + 1]
    chunks, each, _ = same_ref.shape
    for t in range(parts[0].shape[0]):
        h, i = t // chunks, t % chunks
        lses = []
        for p in parts:
            tail = p[t, HEAD_WIDTH:, :].astype(jnp.float32)
            lses.append(tail[0:1] + tail[1:2] + tail[2:3])
        top = functools.reduce(jnp.maximum, lses)
        weights = [jnp.exp2(v - top) for v in lses]
        total = functools.reduce(jnp.add, weights)
        out = None
        for p, w in zip(parts, weights):
            term = p[t, :HEAD_WIDTH, :].astype(jnp.float32) * (w / total)
            out = term if out is None else out + term
        out = out.T
        first, second = out[:each], out[each:]
        at = slice(h * HEAD_WIDTH, (h + 1) * HEAD_WIDTH)
        even = at_ref[0] == 0
        same_ref[i, :, at] = jnp.where(even, first, second).astype(jnp.bfloat16)
        other_ref[i, :, at] = jnp.where(even, second, first).astype(jnp.bfloat16)


def merge(where, parts, tokens, heads):
    chunks = tokens // QB
    each = QB // 2
    return pl.pallas_call(
        functools.partial(merge_kernel, n=len(parts)),
        in_specs=[pl.BlockSpec(memory_space=pltpu.SMEM)] + [pl.BlockSpec(memory_space=pltpu.VMEM)] * len(parts),
        out_specs=[pl.BlockSpec(memory_space=pltpu.VMEM)] * 2,
        out_shape=[jax.ShapeDtypeStruct((chunks, each, heads * HEAD_WIDTH), jnp.bfloat16)] * 2,
        compiler_params=pltpu.CompilerParams(vmem_limit_bytes=LIMIT),
        name="merge",
    )(where, *parts)


SIDE = 4


def sp_shift(dz, dy):
    return [
        (z * SIDE + y, ((z + dz) % SIDE) * SIDE + (y + dy) % SIDE) for z in range(SIDE) for y in range(SIDE)
    ]


def send(x, dz, dy):
    return lax.ppermute(x, "sp", sp_shift(dz, dy))


def front_kernel(at_ref, *refs, blocks, members):
    attn_refs = refs[: 2 * members]
    refs = refs[2 * members :]
    res_refs = refs[:members]
    wo_ref, gain_ref, own_ref, other_ref, act_ref, mid_out_ref, lhs, mid = refs[members:]
    i = pl.program_id(0)
    _, each, width = attn_refs[0].shape
    _, model = lhs.shape
    block = model // blocks

    @pl.when(i == 0)
    def _():
        core, x = at_ref[0], at_ref[1]
        for n, attn_ref in enumerate(attn_refs):
            part = ((x + members - n // 2) % members) * 2 + (1 - core if n % 2 else core)
            at = pl.ds(pl.multiple_of(part * width, width), width)
            for m in range(members):
                lhs[m * each : (m + 1) * each, at] = attn_ref[(x + m) % members]

    @pl.when(i < blocks)
    def _():
        product = jnp.dot(lhs[...], wo_ref[...], preferred_element_type=jnp.float32)
        for m, res in enumerate(res_refs):
            at = slice(m * each, (m + 1) * each)
            mid[i, at, :] = res[...].astype(jnp.float32) + product[at]

    @pl.when(i == blocks)
    def _():
        for r in range(members):
            at = slice(r * each, (r + 1) * each)
            squares = None
            for n in range(blocks):
                for c in range(block // 128):
                    m = mid[n, at, c * 128 : (c + 1) * 128]
                    squares = m * m if squares is None else squares + m * m
            scale = lax.rsqrt(jnp.sum(squares, axis=-1, keepdims=True) * (1.0 / model) + epsilon)
            for n in range(blocks):
                gain = gain_ref[:, n * block : (n + 1) * block]
                lhs[at, n * block : (n + 1) * block] = (mid[n, at, :] * scale * gain).astype(jnp.bfloat16)
        for n in range(blocks):
            mid_out_ref[:, n * block : (n + 1) * block] = mid[n, :each, :]

    def hidden(g_ref):
        h = jnp.dot(lhs[...], g_ref[...].reshape(model, block), preferred_element_type=jnp.float32)
        h = jnp.maximum(h, 0.0)
        act_ref[...] = (h * h).astype(jnp.bfloat16).reshape(members, each, block)

    @pl.when((i >= blocks) & (i < blocks + blocks // 2))
    def _():
        hidden(own_ref)

    @pl.when(i >= blocks + blocks // 2)
    def _():
        hidden(other_ref)


def front(where, attn, residuals, out_weight, norm_gain, own, other, blocks=4):
    members, each, width = attn[0].shape
    model = out_weight.shape[1]
    rows = members * each
    block = model // blocks
    half = blocks // 2
    weight = lambda first: pl.BlockSpec(
        (own.shape[0], each, block), lambda i, a: (0, 0, jnp.clip(i - first, 0, half - 1))
    )
    return pl.pallas_call(
        functools.partial(front_kernel, blocks=blocks, members=members),
        grid_spec=pltpu.PrefetchScalarGridSpec(
            num_scalar_prefetch=1,
            grid=(2 * blocks,),
            in_specs=[
                pl.BlockSpec((members, each, width), lambda i, a: (0, 0, 0)),
            ]
            * len(attn)
            + [pl.BlockSpec((each, block), lambda i, a: (0, jnp.minimum(i, blocks - 1)))] * members
            + [
                pl.BlockSpec((model, block), lambda i, a: (0, jnp.minimum(i, blocks - 1))),
                pl.BlockSpec((1, model), lambda i, a: (0, 0)),
                weight(blocks),
                weight(blocks + half),
            ],
            out_specs=[
                pl.BlockSpec((members, each, block), lambda i, a: (0, 0, jnp.maximum(i - blocks, 0))),
                pl.BlockSpec((each, model), lambda i, a: (0, 0)),
            ],
            scratch_shapes=[
                pltpu.VMEM((rows, model), jnp.bfloat16),
                pltpu.VMEM((blocks, rows, block), jnp.float32),
            ],
        ),
        out_shape=[
            jax.ShapeDtypeStruct((members, each, blocks * block), jnp.bfloat16),
            jax.ShapeDtypeStruct((each, model), jnp.float32),
        ],
        compiler_params=pltpu.CompilerParams(vmem_limit_bytes=LIMIT),
        name="front",
    )(where, *attn, *residuals, out_weight, norm_gain[None], own, other)


def down_kernel(*refs, n_act, n_out):
    act_refs = refs[:n_act]
    own_ref, other_ref = refs[n_act : n_act + 2]
    o_refs = refs[n_act + 2 : n_act + 2 + n_out]
    lhs, w_ref = refs[n_act + 2 + n_out :]
    each = act_refs[0].shape[0]
    half = lhs.shape[1] // 2
    shards = own_ref.shape[0]

    @pl.when(pl.program_id(0) == 0)
    def _():
        for n, act_ref in enumerate(act_refs):
            lhs[n * each : (n + 1) * each, :] = act_ref[...]

    for n, g_ref in enumerate((own_ref, other_ref)):
        for b in range(half // 128):
            for j in range(shards):
                at = slice(n * half + b * 128, n * half + (b + 1) * 128)
                w_ref[at, j * 128 : (j + 1) * 128] = g_ref[j, :, b * 128 : (b + 1) * 128]
    product = jnp.dot(lhs[...], w_ref[...], preferred_element_type=jnp.float32).astype(jnp.bfloat16)
    rows = lhs.shape[0] // n_out
    for n, o_ref in enumerate(o_refs):
        o_ref[...] = product[n * rows : (n + 1) * rows]


def down(act, picks, own, other, n_out, group=4):
    _, each, width = act.shape
    shards, _, both = own.shape
    rows = len(picks) * each // n_out
    spec = pl.BlockSpec((group, each, both // 2), lambda i: (i, 0, 1))
    return pl.pallas_call(
        functools.partial(down_kernel, n_act=len(picks), n_out=n_out),
        grid=(shards // group,),
        in_specs=[pl.BlockSpec((None, each, width), lambda i, p=p: (p, 0, 0)) for p in picks] + [spec, spec],
        out_specs=[pl.BlockSpec((rows, group * each), lambda i: (0, i))] * n_out,
        out_shape=[jax.ShapeDtypeStruct((rows, shards * each), jnp.bfloat16)] * n_out,
        scratch_shapes=[
            pltpu.VMEM((len(picks) * each, width), jnp.bfloat16),
            pltpu.VMEM((width, group * each), jnp.bfloat16),
        ],
        compiler_params=pltpu.CompilerParams(vmem_limit_bytes=LIMIT),
        name="down",
    )(*[act] * len(picks), own, other)


def local(
    residual_in,
    queries,
    keys,
    values,
    query_gain,
    key_norm_gain,
    out_weight,
    norm_gain,
    up_weight,
    down_weight,
    *,
    sp_size,
    tp_size,
):
    tokens = keys.shape[0]
    heads = queries.shape[1] // HEAD_WIDTH

    def send_x(x, dx):
        pairs = [(t, (t + 2 * dx) % tp_size) for t in range(tp_size)]
        return lax.ppermute(x, "tp", pairs)

    q0, kv0, both = prep(
        queries, keys, values, query_gain, key_norm_gain, up_weight, down_weight, sp_size
    )
    kv_p = send(kv0, 1, 0)
    kv_m = send(kv0, -1, 0)
    q_p = send(q0, 0, 1)
    q_m = send(q0, 0, -1)
    weights = lax.all_gather(both, "sp", axis=0)
    residuals = [residual_in] + [send_x(residual_in, -d) for d in (1, 2, 3)]
    own = flash([q0], [kv0], step=1024)
    half_k, half_q = tokens // 2, q0.shape[0] // 2
    kv_2a = send(kv_p[:, :half_k], 1, 0)
    kv_2b = send(kv_m[:, half_k:], -1, 0)
    q_2a = send(q_p[:half_q], 0, 1)
    q_2b = send(q_m[half_q:], 0, -1)
    kv_all = [kv0, kv_p, kv_m, kv_2a, kv_2b]
    far = flash([q_2a, q_2b], kv_all, step=4096)
    back_far = send(far, 0, 2)
    q_p, q_m, far = lax.optimization_barrier((q_p, q_m, far))
    near_p, near_m = flash([q_p, q_m], kv_all, 2, step=4096)
    back_p = send(near_p, 0, -1)
    back_m = send(near_m, 0, 1)
    own, near_p = lax.optimization_barrier((own, near_p))
    own = flash([q0], kv_all[1:], 1, (own,), step=3072)
    index = lax.axis_index("tp").astype(jnp.int32)
    where = jnp.stack([index % 2, index // 2])
    same, other = merge(where, [own, back_p, back_m, back_far], tokens, heads)
    weights, _ = lax.optimization_barrier((weights, same))
    all_heads = [same]
    for n in range(1, tp_size):
        pairs = [(t, (t + 2 * (n // 2)) % tp_size ^ (n % 2)) for t in range(tp_size)]
        all_heads.append(lax.ppermute(other if n % 2 else same, "tp", pairs))
    other_weights = lax.ppermute(weights, "tp", [(t, t ^ 1) for t in range(tp_size)])
    act, middle = front(where, all_heads, residuals, out_weight, norm_gain, weights, other_weights)
    far_sum = down(act, [2], weights, other_weights, 1)[0]
    from_far = send_x(far_sum, 2)
    far_sum, act = lax.optimization_barrier((far_sum, act))
    mine_sum, up_sum, low_sum = down(act, [0, 1, 3], weights, other_weights, 3)
    wide = lambda x: x.astype(jnp.float32)
    from_low = send_x(up_sum, 1)
    from_up = send_x(low_sum, -1)
    return (middle + wide(mine_sum) + wide(from_low) + wide(from_up) + wide(from_far)).astype(jnp.bfloat16)


def solution(mesh):
    return jax.shard_map(
        functools.partial(local, sp_size=mesh.shape["sp"], tp_size=mesh.shape["tp"]),
        mesh=mesh,
        in_specs=(
            P(("sp", "tp"), None),
            P("sp", "tp"),
            P("sp", "tp"),
            P("sp", "tp"),
            P(),
            P(),
            P(),
            P(),
            P("sp", "tp"),
            P("tp", "sp"),
        ),
        out_specs=P(("sp", "tp"), None),
        check_vma=False,
    )
```
